512 devices in a mesh: gr: 2 (over z_hi), sp: 32 (over z_lo, y), tp: 8 (over x, core).
Axes of the slice: x: 4, y: 8, z: 8 (z_hi: 2, z_lo: 4; z = z_hi * 4 + z_lo), core: 2. Of those that a mesh axis runs over, the one named last changes fastest.
Arguments:
- mixer_input: bfloat16 [64, 6144, 2048], P(('gr', 'tp'), 'sp'), may hold values from -16.8 to 16.8
- key_weight: bfloat16 [2048, 256], P('tp'), may hold values from -0.125 to 0.125
- content_projection_matrix: bfloat16 [2048, 256], P('tp'), may hold values from -0.125 to 0.125
- new_queries: bfloat16 [64, 32, 64], P(('gr', 'sp'), 'tp'), may hold values from -6 to 6
- head_stick_offset: float32 [32], replicated, may hold values from -11 to -4
Outputs:
- kv_cache: bfloat16 [64, 8, 6144, 128], P(('gr', 'sp'), 'tp')
- initial_attended_output: bfloat16 [64, 32, 64], P(('gr', 'sp'), 'tp')
The draws below stay inside these ranges and needn't reach their ends.
All inputs are finite; a program needn't handle non-finite values.
Results may differ from the reference program's by a relative error of at most 0.0081.
Values may be sent and summed in bfloat16 or wider, within the bound.
No kernel may reach another device: no remote copies, remote signals or barrier semaphores. Data moves between devices by JAX's collectives and lax.ppermute only.
A program may use at most 64 MiB of HBM per device.

```python
import jax
import jax.numpy as jnp
from jax import lax

D = 2048
HEADS = 32
KV_HEADS = 4
HEAD_DIM = 64
BLOCK_POS = 192
CONTEXT_SPAN = 6144
BATCH_COUNT = 64
KV_SLOTS = 8


def draw_mixer_input(key, part):
    base_key = jax.random.fold_in(key, 11)
    scale_key = jax.random.fold_in(key, 12)
    arrival_draw_seed = jax.random.fold_in(key, 13)
    lookup_cells = jnp.clip(jax.random.normal(base_key, (BATCH_COUNT, CONTEXT_SPAN, D), jnp.float32), -4.0, 4.0)
    block_scale = jnp.exp(jax.random.uniform(scale_key, (BATCH_COUNT, CONTEXT_SPAN // BLOCK_POS, 1, 1), jnp.float32, jnp.log(0.35), jnp.log(1.4)))
    lookup_cells = (lookup_cells.reshape(BATCH_COUNT, CONTEXT_SPAN // BLOCK_POS, BLOCK_POS, D) * block_scale).reshape(BATCH_COUNT, CONTEXT_SPAN, D)
    arrival_clusters = jax.random.bernoulli(arrival_draw_seed, 4.0 / CONTEXT_SPAN, (BATCH_COUNT, CONTEXT_SPAN, 1))
    lookup_cells = lookup_cells * jnp.where(arrival_clusters, 3.0, 1.0)
    return lookup_cells.astype(jnp.bfloat16)


def draw_head_stick_offset(key, part):
    offset_key = jax.random.fold_in(key, 21)
    values_drawn = jax.random.uniform(offset_key, (HEADS,), jnp.float32, -9.5, -4.0)
    return values_drawn.astype(jnp.float32)


def levels(own_key, extent, pieces, smallest, high):
    def one(position, parts):
        steps = jax.random.uniform(jax.random.fold_in(jax.random.fold_in(own_key, 6), position), (parts,), jnp.float32, smallest / len(pieces), high / len(pieces))
        return jnp.repeat(jnp.exp(steps), extent[position] // parts).reshape((-1,) + (1,) * (len(extent) - position - 1))

    factor_of = one(*pieces[0])
    for cut in pieces[1:]:
        factor_of = factor_of * one(*cut)
    return factor_of


def centred(rng, dims, deviation, most, shards=(), held_as=jnp.bfloat16):
    array = deviation * jax.random.normal(rng, dims, jnp.float32)
    if shards:
        array = array * levels(rng, dims, shards, -0.22, 0.18)
    return jnp.clip(array, -most, most).astype(held_as)


def setup_inputs(seed: int = 0) -> dict:
    keys = jax.random.split(jax.random.key(seed), 6)
    mixer_input = draw_mixer_input(jax.random.fold_in(keys[5], 71), 0)
    key_weight = centred(keys[1], (D, KV_HEADS * HEAD_DIM), D ** -0.5, 0.125, ((0, 8),))
    content_projection_matrix = centred(keys[2], (D, KV_HEADS * HEAD_DIM), D ** -0.5, 0.125, ((0, 8),))
    new_queries = centred(keys[3], (BATCH_COUNT, HEADS, HEAD_DIM), 1.0, 6.0, ((0, 64), (1, 8)))
    head_stick_offset = draw_head_stick_offset(jax.random.fold_in(keys[5], 71), 0)
    return {"mixer_input": mixer_input, "key_weight": key_weight, "content_projection_matrix": content_projection_matrix, "new_queries": new_queries, "head_stick_offset": head_stick_offset}


def reference(mixer_input, key_weight, content_projection_matrix, new_queries, head_stick_offset):
    key_heads = key_weight.shape[1] // HEAD_DIM
    copies = KV_SLOTS // key_heads
    per_group = HEADS // key_heads
    offset_values = head_stick_offset.reshape(key_heads, per_group, 1)

    def one_sequence(operands):
        input_rows, query_rows = operands
        key_rows = jnp.dot(input_rows, key_weight, preferred_element_type=jnp.float32).astype(jnp.bfloat16)
        value_rows = jnp.dot(input_rows, content_projection_matrix, preferred_element_type=jnp.float32).astype(jnp.bfloat16)
        key_rows = key_rows.reshape(CONTEXT_SPAN, key_heads, HEAD_DIM).transpose(1, 0, 2)
        value_rows = value_rows.reshape(CONTEXT_SPAN, key_heads, HEAD_DIM).transpose(1, 0, 2)
        stacked = jnp.concatenate([key_rows, value_rows], axis=2)
        cache_rows = jnp.repeat(stacked, copies, axis=0)
        grouped = query_rows.reshape(key_heads, per_group, HEAD_DIM).astype(jnp.float32)
        logit_scores = jnp.einsum('hgd,hsd->hgs', grouped, key_rows.astype(jnp.float32)) * HEAD_DIM ** -0.5 + offset_values
        stay_terms = jax.nn.log_sigmoid(-logit_scores)
        later_terms = lax.cumsum(stay_terms, axis=2, reverse=True) - stay_terms
        weights = jnp.exp(jax.nn.log_sigmoid(logit_scores) + later_terms).astype(jnp.bfloat16)
        result = jnp.einsum('hgs,hsd->hgd', weights.astype(jnp.float32), value_rows.astype(jnp.float32))
        return cache_rows, result.reshape(HEADS, HEAD_DIM).astype(jnp.bfloat16)

    kv_cache, initial_attended_output = lax.map(one_sequence, (mixer_input, new_queries))
    return kv_cache, initial_attended_output
```

```python
import functools

import jax
import jax.numpy as jnp
from jax import lax
from jax.experimental import pallas as pl
from jax.experimental.pallas import tpu as pltpu
from jax.sharding import Mesh, PartitionSpec as P

HEAD_DIM = 64
F32, BF16 = jnp.float32, jnp.bfloat16


def project_kernel(core_ref, x_ref, mine_ref, other_ref, out_ref):
    shards, depth, width = mine_ref.shape
    seqs, half = out_ref.shape[1], out_ref.shape[2]
    core = core_ref[0]
    total = None
    for s in range(shards):
        for ref, which in ((mine_ref, core), (other_ref, 1 - core)):
            at = pl.multiple_of((2 * s + which) * depth, depth)
            part = jnp.dot(x_ref[:, pl.ds(at, depth)], ref[s], preferred_element_type=F32)
            total = part if total is None else total + part
    rows = total.astype(BF16)
    for slot in range(out_ref.shape[0]):
        for i in range(seqs):
            start = (2 * i + slot % 2) * half
            head = slot // 2
            out_ref[slot, i] = rows[start : start + half, 128 * head : 128 * head + 128]


def project(core, x, mine, other, seqs, half):
    heads = mine.shape[2] // 128
    return pl.pallas_call(
        project_kernel,
        out_shape=jax.ShapeDtypeStruct((2 * heads, seqs, half, 128), BF16),
        in_specs=[pl.BlockSpec(memory_space=pltpu.SMEM)] + [pl.BlockSpec(memory_space=pltpu.VMEM)] * 3,
        out_specs=pl.BlockSpec(memory_space=pltpu.VMEM),
        cost_estimate=pl.CostEstimate(flops=2 * x.shape[0] * x.shape[1] * mine.shape[2], bytes_accessed=8 << 20, transcendentals=0),
    )(core, x, mine, other)


def split3(a):
    hi = a.astype(BF16)
    rest = a - hi.astype(F32)
    mid = rest.astype(BF16)
    return hi, mid, (rest - mid.astype(F32)).astype(BF16)


def read_kernel(core_ref, mine_ref, other_ref, q_ref, off_ref, kv_ref, out_ref):
    blocks, half, width = mine_ref.shape
    span = kv_ref.shape[2]
    rows = q_ref.shape[0]
    core = core_ref[0]
    for b in range(blocks):
        base = 2 * half * b
        kv_ref[0, 0, pl.ds(pl.multiple_of(base + core * half, half), half)] = mine_ref[b]
        kv_ref[0, 0, pl.ds(pl.multiple_of(base + (1 - core) * half, half), half)] = other_ref[b]
    tiles = span // 128
    scores = lax.dot_general(q_ref[...], kv_ref[0, 0], (((1,), (1,)), ((), ())), preferred_element_type=F32)
    z = scores * (HEAD_DIM ** -0.5) + off_ref[:, :1]
    stay = -(jnp.maximum(z, 0.0) + jnp.log1p(jnp.exp(-jnp.abs(z))))
    stacked = jnp.concatenate([stay[:, 128 * t : 128 * t + 128] for t in range(tiles)], axis=0)
    r = lax.broadcasted_iota(jnp.int32, (128, 128), 0)
    c = lax.broadcasted_iota(jnp.int32, (128, 128), 1)
    from_here = (r >= c).astype(F32).astype(BF16)
    suffix = None
    for piece in split3(stacked):
        part = jnp.dot(piece, from_here, preferred_element_type=F32)
        suffix = part if suffix is None else suffix + part
    later = jnp.zeros((rows, 1), F32)
    pieces = [None] * tiles
    for t in reversed(range(tiles)):
        own = suffix[rows * t : rows * t + rows]
        pieces[t] = own + later
        later = later + own[:, :1]
    log_weight = z + jnp.concatenate(pieces, axis=1)
    weight = jnp.exp(log_weight).astype(BF16)
    out_ref[...] = jnp.dot(weight, kv_ref[0, 0], preferred_element_type=F32)


def read(core, mine, other, q, off):
    blocks, half, width = mine.shape
    span = 2 * blocks * half
    rows = q.shape[0]
    return pl.pallas_call(
        read_kernel,
        out_shape=(jax.ShapeDtypeStruct((1, 1, span, width), BF16), jax.ShapeDtypeStruct((rows, width), F32)),
        in_specs=[pl.BlockSpec(memory_space=pltpu.SMEM)] + [pl.BlockSpec(memory_space=pltpu.VMEM)] * 4,
        out_specs=(pl.BlockSpec(memory_space=pltpu.VMEM), pl.BlockSpec(memory_space=pltpu.VMEM)),
        cost_estimate=pl.CostEstimate(flops=4 * rows * span * width, bytes_accessed=4 << 20, transcendentals=3 * rows * span),
    )(core, mine, other, q, off)


def local(mixer_input, key_weight, content_projection_matrix, new_queries, head_stick_offset):
    seqs, block, width = mixer_input.shape
    depth, columns = key_weight.shape
    heads = columns // HEAD_DIM
    half = block // 2
    core = lax.axis_index("core")
    core_arg = core.reshape(1).astype(jnp.int32)
    other = [(0, 1), (1, 0)]
    weight = jnp.concatenate(
        [key_weight.reshape(depth, heads, HEAD_DIM), content_projection_matrix.reshape(depth, heads, HEAD_DIM)], axis=2
    ).reshape(depth, 2 * columns)
    chips = lax.axis_size("x")
    mine = lax.all_to_all(jnp.broadcast_to(weight, (chips, *weight.shape)), "x", 0, 0, tiled=True)
    theirs = lax.ppermute(mine, "core", other)
    rows = project(core_arg, mixer_input.reshape(seqs * block, width), mine, theirs, seqs, half)
    rows = lax.all_to_all(rows, ("x", "core"), 0, 0, tiled=True)
    rows = rows.reshape(rows.shape[0] * seqs, half, 128)
    mine = lax.all_to_all(rows, ("z", "y"), 0, 0, tiled=True)
    theirs = lax.ppermute(mine, "core", other)
    group = new_queries.shape[1]
    start = (lax.axis_index("x") * 2 + core) * group
    offset = lax.dynamic_slice_in_dim(head_stick_offset, start, group)
    q = jnp.pad(new_queries[0], ((0, 8 - group), (0, 128 - HEAD_DIM)))
    off = jnp.broadcast_to(jnp.pad(offset, (0, 8 - group))[:, None], (8, 128))
    kv_cache, read_out = read(core_arg, mine, theirs, q, off)
    return kv_cache, read_out[None, :group, HEAD_DIM:].astype(BF16)


def solution(mesh):
    sizes = dict(mesh.shape)
    wide = Mesh(mesh.devices.reshape(sizes["gr"], 4, 8, 4, 2), ("gr", "z", "y", "x", "core"))
    sp, tp = ("z", "y"), ("x", "core")
    return jax.shard_map(
        local,
        mesh=wide,
        in_specs=(
            P(("gr", *tp), sp, None),
            P(tp, None),
            P(tp, None),
            P(("gr", *sp), tp, None),
            P(),
        ),
        out_specs=(P(("gr", *sp), tp, None, None), P(("gr", *sp), tp, None)),
        check_vma=False,
    )
```

```python
import jax
import jax.numpy as jnp
from jax import lax
from jax.experimental import pallas as pl
from jax.experimental.pallas import tpu as pltpu
from jax.sharding import Mesh, PartitionSpec as P

HEAD_DIM = 64
F32, BF16 = jnp.float32, jnp.bfloat16
SMEM = pl.BlockSpec(memory_space=pltpu.SMEM)
VMEM = pl.BlockSpec(memory_space=pltpu.VMEM)
ANY = pl.BlockSpec(memory_space=pl.ANY)


def project_kernel(core_ref, mine_ref, other_ref, w_ref, out_ref):
    core = core_ref[0]
    heads, both, half, _ = out_ref.shape
    seq = pl.program_id(0)
    for ref, which in ((mine_ref, core), (other_ref, 1 - core)):
        rows = jnp.dot(ref[...], w_ref[...], preferred_element_type=F32)
        for h in range(heads):
            part = rows[:, HEAD_DIM * h : HEAD_DIM * h + HEAD_DIM]
            out_ref[h, which * (both // 2) + seq] = jnp.concatenate([part[:half], part[half:]], axis=1).astype(BF16)


def project(core, mine, other, w, seqs, half):
    heads = w.shape[1] // HEAD_DIM
    rows = pl.BlockSpec((2 * half, w.shape[0]), lambda i: (i, 0))
    return pl.pallas_call(
        project_kernel,
        out_shape=jax.ShapeDtypeStruct((heads, 2 * seqs, half, 128), BF16),
        grid=(seqs,),
        in_specs=[SMEM, rows, rows, pl.BlockSpec(w.shape, lambda i: (0, 0))],
        out_specs=pl.BlockSpec((heads, 2 * seqs, half, 128), lambda i: (0, 0, 0, 0)),
        compiler_params=pltpu.CompilerParams(vmem_limit_bytes=24 << 20),
        cost_estimate=pl.CostEstimate(flops=4 * mine.shape[0] * w.shape[0] * w.shape[1], bytes_accessed=8 << 20, transcendentals=0),
    )(core, mine, other, w)


def split3(a):
    hi = a.astype(BF16)
    rest = a - hi.astype(F32)
    mid = rest.astype(BF16)
    return hi, mid, (rest - mid.astype(F32)).astype(BF16)


PARTS = 4


def read_kernel(info_ref, off_ref, mine_ref, other_ref, q_ref, cache_ref, out_ref, kv_ref, sems):
    blocks, half, width = mine_ref.shape
    span = kv_ref.shape[0]
    group = q_ref.shape[1]
    core, first = info_ref[0], info_ref[1]
    swap = core == 1
    piece = span // PARTS
    copies = []
    for b in range(blocks):
        a, o = mine_ref[b], other_ref[b]
        keys = jnp.where(swap, o, a)
        values = jnp.where(swap, a, o)
        base = 2 * half * b
        kv_ref[pl.ds(base, half)] = jnp.concatenate([keys[:, :HEAD_DIM], values[:, :HEAD_DIM]], axis=1)
        kv_ref[pl.ds(base + half, half)] = jnp.concatenate([keys[:, HEAD_DIM:], values[:, HEAD_DIM:]], axis=1)
        done = base + 2 * half
        if done % piece == 0:
            n = done // piece - 1
            copy = pltpu.make_async_copy(
                kv_ref.at[pl.ds(n * piece, piece)], cache_ref.at[0, 0, pl.ds(n * piece, piece)], sems.at[n]
            )
            copy.start()
            copies.append(copy)
    tiles = span // 128
    rows = 8
    q = jnp.concatenate([q_ref[0], jnp.zeros((group, width - HEAD_DIM), BF16)], axis=1)
    q = jnp.concatenate([q, jnp.zeros((rows - group, width), BF16)], axis=0)
    row = lax.broadcasted_iota(jnp.int32, (rows, 128), 0)
    off = jnp.zeros((rows, 128), F32)
    for g in range(group):
        off = jnp.where(row == g, off_ref[first + g], off)
    scores = lax.dot_general(q, kv_ref[...], (((1,), (1,)), ((), ())), preferred_element_type=F32)
    z = scores * (HEAD_DIM ** -0.5) + off[:, :1]
    stay = -(jnp.maximum(z, 0.0) + jnp.log1p(jnp.exp(-jnp.abs(z))))
    stacked = jnp.concatenate([stay[:, 128 * t : 128 * t + 128] for t in range(tiles)], axis=0)
    r = lax.broadcasted_iota(jnp.int32, (128, 128), 0)
    c = lax.broadcasted_iota(jnp.int32, (128, 128), 1)
    from_here = (r >= c).astype(F32).astype(BF16)
    suffix = None
    for part in split3(stacked):
        part = jnp.dot(part, from_here, preferred_element_type=F32)
        suffix = part if suffix is None else suffix + part
    later = jnp.zeros((rows, 1), F32)
    pieces = [None] * tiles
    for t in reversed(range(tiles)):
        own = suffix[rows * t : rows * t + rows]
        pieces[t] = own + later
        later = later + own[:, :1]
    weight = jnp.exp(z + jnp.concatenate(pieces, axis=1)).astype(BF16)
    out = jnp.dot(weight, kv_ref[...], preferred_element_type=F32)
    out_ref[0] = out[:group, HEAD_DIM:].astype(BF16)
    for copy in copies:
        copy.wait()


def read(info, off, mine, other, q):
    blocks, half, width = mine.shape
    span = 2 * blocks * half
    group = q.shape[1]
    return pl.pallas_call(
        read_kernel,
        out_shape=(jax.ShapeDtypeStruct((1, 1, span, width), BF16), jax.ShapeDtypeStruct(q.shape, BF16)),
        in_specs=[SMEM, SMEM, VMEM, VMEM, VMEM],
        out_specs=(ANY, VMEM),
        scratch_shapes=[pltpu.VMEM((span, width), BF16), pltpu.SemaphoreType.DMA((PARTS,))],
        compiler_params=pltpu.CompilerParams(vmem_limit_bytes=24 << 20),
        cost_estimate=pl.CostEstimate(flops=32 * span * width, bytes_accessed=4 << 20, transcendentals=24 * span),
    )(info, off, mine, other, q)


def local(mixer_input, key_weight, content_projection_matrix, new_queries, head_stick_offset):
    seqs, block, width = mixer_input.shape
    depth, columns = key_weight.shape
    half = block // 2
    core = lax.axis_index("core").astype(jnp.int32)
    other = [(0, 1), (1, 0)]
    rows = mixer_input.reshape(seqs * block, width)
    their_rows = lax.ppermute(rows, "core", other)
    chips = lax.axis_size("x")
    weight = jnp.stack([key_weight, content_projection_matrix])
    weight = jnp.broadcast_to(weight, (chips, *weight.shape)).reshape(2 * chips, depth, columns)
    weight = lax.all_to_all(weight, ("x", "core"), 0, 0, tiled=True).reshape(2 * chips * depth, columns)
    packed = project(core.reshape(1), rows, their_rows, weight, seqs, half)
    packed = lax.all_to_all(packed, "x", 0, 0, tiled=True)
    packed = packed.reshape(packed.shape[0] * 2 * seqs, half, 128)
    mine = lax.all_to_all(packed, ("z", "y"), 0, 0, tiled=True)
    theirs = lax.ppermute(mine, "core", other)
    first = (lax.axis_index("x") * 2 + core) * new_queries.shape[1]
    return read(jnp.stack([core, first]), head_stick_offset, mine, theirs, new_queries)


def solution(mesh):
    wide = Mesh(mesh.devices.reshape(2, 4, 8, 4, 2), ("gr", "z", "y", "x", "core"))
    sp, tp = ("z", "y"), ("x", "core")
    return jax.shard_map(
        local,
        mesh=wide,
        in_specs=(P(("gr", *tp), sp, None), P(tp, None), P(tp, None), P(("gr", *sp), tp, None), P()),
        out_specs=(P(("gr", *sp), tp, None, None), P(("gr", *sp), tp, None)),
        check_vma=False,
    )
```

```python
import jax
import jax.numpy as jnp
from jax import lax
from jax.experimental import pallas as pl
from jax.experimental.pallas import tpu as pltpu
from jax.sharding import Mesh, PartitionSpec as P

HEAD_DIM = 64
F32, BF16 = jnp.float32, jnp.bfloat16
SMEM = pl.BlockSpec(memory_space=pltpu.SMEM)
VMEM = pl.BlockSpec(memory_space=pltpu.VMEM)
HBM = pl.BlockSpec(memory_space=pltpu.HBM)
GRANT = pltpu.CompilerParams(vmem_limit_bytes=20 << 20)


def first_kernel(core_ref, x_ref, w_ref, sum_ref, rows_ref, sems):
    core = core_ref[0]
    shards, depth, _ = w_ref.shape
    copies = []
    for which in (core, 1 - core):
        for s in range(shards):
            at = pl.ds(pl.multiple_of((2 * s + which) * depth, depth), depth)
            copy = pltpu.make_async_copy(x_ref.at[:, at], rows_ref.at[:, at], sems.at[len(copies)])
            copy.start()
            copies.append((copy, at))
    total = None
    for s in range(shards):
        copy, at = copies[s]
        copy.wait()
        part = jnp.dot(rows_ref[:, at], w_ref[s], preferred_element_type=F32)
        total = part if total is None else total + part
    sum_ref[...] = total
    for copy, _ in copies[shards:]:
        copy.wait()


def second_kernel(core_ref, rows_ref, w_ref, sum_ref, out_ref):
    core = core_ref[0]
    shards, depth, width = w_ref.shape
    slots, seqs, half, _ = out_ref.shape
    total = sum_ref[...]
    for s in range(shards):
        at = pl.multiple_of((2 * s + 1 - core) * depth, depth)
        total = total + jnp.dot(rows_ref[:, pl.ds(at, depth)], w_ref[s], preferred_element_type=F32)
    rows = total.astype(BF16)
    for slot in range(slots):
        for i in range(seqs):
            start, key = (2 * i + slot % 2) * half, HEAD_DIM * (slot // 2)
            value = key + width // 2
            part = rows[start : start + half]
            out_ref[slot, i] = jnp.concatenate([part[:, key : key + HEAD_DIM], part[:, value : value + HEAD_DIM]], axis=1)


def first(core, x, w):
    shards, depth, width = w.shape
    return pl.pallas_call(
        first_kernel,
        out_shape=(jax.ShapeDtypeStruct((x.shape[0], width), F32), jax.ShapeDtypeStruct(x.shape, BF16)),
        in_specs=[SMEM, HBM, VMEM],
        out_specs=(VMEM, VMEM),
        scratch_shapes=[pltpu.SemaphoreType.DMA((2 * shards,))],
        compiler_params=GRANT,
        cost_estimate=pl.CostEstimate(flops=x.shape[0] * x.shape[1] * width, bytes_accessed=4 << 20, transcendentals=0),
    )(core, x, w)


def second(core, rows, w, total, seqs, half):
    slots = w.shape[2] // HEAD_DIM
    return pl.pallas_call(
        second_kernel,
        out_shape=jax.ShapeDtypeStruct((slots, seqs, half, 2 * HEAD_DIM), BF16),
        in_specs=[SMEM, VMEM, VMEM, VMEM],
        out_specs=VMEM,
        compiler_params=GRANT,
        cost_estimate=pl.CostEstimate(flops=rows.shape[0] * rows.shape[1] * w.shape[2], bytes_accessed=4 << 20, transcendentals=0),
    )(core, rows, w, total)


def split3(a):
    hi = a.astype(BF16)
    rest = a - hi.astype(F32)
    mid = rest.astype(BF16)
    return hi, mid, (rest - mid.astype(F32)).astype(BF16)


def read_kernel(core_ref, first_ref, off_ref, mine_ref, other_ref, q_ref, cache_ref, out_ref, kv_ref, sems):
    blocks, half, width = mine_ref.shape
    span = kv_ref.shape[0]
    group = q_ref.shape[1]
    core, first_head = core_ref[0], first_ref[0]
    copies = []
    for ref, which in ((mine_ref, core), (other_ref, 1 - core)):
        copy = pltpu.make_async_copy(ref, cache_ref.at[:, which], sems.at[len(copies)])
        copy.start()
        copies.append(copy)
    for b in range(blocks):
        base = 2 * half * b
        kv_ref[pl.ds(pl.multiple_of(base + core * half, half), half)] = mine_ref[b]
        kv_ref[pl.ds(pl.multiple_of(base + (1 - core) * half, half), half)] = other_ref[b]
    tiles = span // 128
    rows = 8
    q = jnp.concatenate([q_ref[0], jnp.zeros((group, width - HEAD_DIM), BF16)], axis=1)
    q = jnp.concatenate([q, jnp.zeros((rows - group, width), BF16)], axis=0)
    row = lax.broadcasted_iota(jnp.int32, (rows, 128), 0)
    off = jnp.zeros((rows, 128), F32)
    for g in range(group):
        off = jnp.where(row == g, off_ref[first_head + g], off)
    scores = lax.dot_general(q, kv_ref[...], (((1,), (1,)), ((), ())), preferred_element_type=F32)
    z = scores * (HEAD_DIM ** -0.5) + off[:, :1]
    stay = -(jnp.maximum(z, 0.0) + jnp.log1p(jnp.exp(-jnp.abs(z))))
    stacked = jnp.concatenate([stay[:, 128 * t : 128 * t + 128] for t in range(tiles)], axis=0)
    r = lax.broadcasted_iota(jnp.int32, (128, 128), 0)
    c = lax.broadcasted_iota(jnp.int32, (128, 128), 1)
    from_here = (r >= c).astype(F32).astype(BF16)
    suffix = None
    for part in split3(stacked):
        part = jnp.dot(part, from_here, preferred_element_type=F32)
        suffix = part if suffix is None else suffix + part
    later = jnp.zeros((rows, 1), F32)
    pieces = [None] * tiles
    for t in reversed(range(tiles)):
        own = suffix[rows * t : rows * t + rows]
        pieces[t] = own + later
        later = later + own[:, :1]
    weight = jnp.exp(z + jnp.concatenate(pieces, axis=1)).astype(BF16)
    out = jnp.dot(weight, kv_ref[...], preferred_element_type=F32)
    out_ref[0] = out[:group, HEAD_DIM:].astype(BF16)
    for copy in copies:
        copy.wait()


def read(core, first_head, off, mine, other, q):
    blocks, half, width = mine.shape
    span = 2 * blocks * half
    cache, out = pl.pallas_call(
        read_kernel,
        out_shape=(jax.ShapeDtypeStruct((blocks, 2, half, width), BF16), jax.ShapeDtypeStruct(q.shape, BF16)),
        in_specs=[SMEM, SMEM, SMEM, VMEM, VMEM, VMEM],
        out_specs=(HBM, VMEM),
        scratch_shapes=[pltpu.VMEM((span, width), BF16), pltpu.SemaphoreType.DMA((2,))],
        compiler_params=GRANT,
        cost_estimate=pl.CostEstimate(flops=32 * span * width, bytes_accessed=4 << 20, transcendentals=24 * span),
    )(core, first_head, off, mine, other, q)
    return cache.reshape(1, 1, span, width), out


def local(mixer_input, key_weight, content_projection_matrix, new_queries, head_stick_offset):
    seqs, block, width = mixer_input.shape
    half = block // 2
    core = lax.axis_index("core").astype(jnp.int32)
    core_arg = core.reshape(1)
    first_head = ((lax.axis_index("x") * 2 + core) * new_queries.shape[1]).reshape(1)
    swap = [(0, 1), (1, 0)]
    weight = jnp.concatenate([key_weight, content_projection_matrix], axis=1)
    weight = jnp.broadcast_to(weight, (lax.axis_size("x"), *weight.shape))
    mine = lax.all_to_all(weight, "x", 0, 0, tiled=True)
    theirs = lax.ppermute(mine, "core", swap)
    total, rows = first(core_arg, mixer_input.reshape(seqs * block, width), mine)
    packed = second(core_arg, rows, theirs, total, seqs, half)
    packed = lax.all_to_all(packed, ("x", "core"), 0, 0, tiled=True)
    packed = packed.reshape(packed.shape[0] * seqs, half, 2 * HEAD_DIM)
    mine = lax.all_to_all(packed, ("z", "y"), 0, 0, tiled=True)
    theirs = lax.ppermute(mine, "core", swap)
    return read(core_arg, first_head, head_stick_offset, mine, theirs, new_queries)


def solution(mesh):
    wide = Mesh(mesh.devices.reshape(2, 4, 8, 4, 2), ("gr", "z", "y", "x", "core"))
    sp, tp = ("z", "y"), ("x", "core")
    return jax.shard_map(
        local,
        mesh=wide,
        in_specs=(P(("gr", *tp), sp, None), P(tp, None), P(tp, None), P(("gr", *sp), tp, None), P()),
        out_specs=(P(("gr", *sp), tp, None, None), P(("gr", *sp), tp, None)),
        check_vma=False,
    )
```

```python
import jax
import jax.numpy as jnp
from jax import lax
from jax.experimental import pallas as pl
from jax.experimental.pallas import tpu as pltpu
from jax.sharding import Mesh, PartitionSpec as P


HEAD_DIM = 64
F32, BF16 = jnp.float32, jnp.bfloat16
SMEM = pl.BlockSpec(memory_space=pltpu.SMEM)
VMEM = pl.BlockSpec(memory_space=pltpu.VMEM)
HBM = pl.BlockSpec(memory_space=pltpu.HBM)
GRANT = pltpu.CompilerParams(vmem_limit_bytes=16 << 20)


def stage_kernel(x_ref, out_ref, sem):
    copy = pltpu.make_async_copy(x_ref, out_ref, sem)
    copy.start()
    copy.wait()


def stage(x):
    return pl.pallas_call(
        stage_kernel,
        out_shape=jax.ShapeDtypeStruct(x.shape, x.dtype),
        in_specs=[HBM],
        out_specs=VMEM,
        scratch_shapes=[pltpu.SemaphoreType.DMA],
        compiler_params=GRANT,
        cost_estimate=pl.CostEstimate(flops=1 << 30, bytes_accessed=6 << 20, transcendentals=0),
    )(x)


CHUNKS = 4


def project_kernel(core_ref, mine_ref, other_hbm, w_hbm, out_ref, other_ref, w_ref, sems):
    core = core_ref[0]
    heads, both, half, _ = out_ref.shape
    seqs = both // 2
    depth = w_ref.shape[0] // CHUNKS
    cuts = [pl.ds(k * depth, depth) for k in range(CHUNKS)]
    weights = [pltpu.make_async_copy(w_hbm.at[c], w_ref.at[c], sems.at[0, k]) for k, c in enumerate(cuts)]
    others = [pltpu.make_async_copy(other_hbm.at[:, c], other_ref.at[:, c], sems.at[1, k]) for k, c in enumerate(cuts)]
    for copy in weights + others:
        copy.start()
    for ref, which, copies in ((mine_ref, core, weights), (other_ref, 1 - core, others)):
        rows = None
        for c, copy in zip(cuts, copies):
            copy.wait()
            part = jnp.dot(ref[:, c], w_ref[c], preferred_element_type=F32)
            rows = part if rows is None else rows + part
        for i in range(seqs):
            for h in range(heads):
                part = rows[2 * half * i : 2 * half * (i + 1), HEAD_DIM * h : HEAD_DIM * h + HEAD_DIM]
                out_ref[h, which * seqs + i] = jnp.concatenate([part[:half], part[half:]], axis=1).astype(BF16)


def project(core, mine, other, w, seqs, half):
    heads = w.shape[1] // HEAD_DIM
    return pl.pallas_call(
        project_kernel,
        out_shape=jax.ShapeDtypeStruct((heads, 2 * seqs, half, 128), BF16),
        in_specs=[SMEM, VMEM, HBM, HBM],
        out_specs=VMEM,
        scratch_shapes=[pltpu.VMEM(other.shape, BF16), pltpu.VMEM(w.shape, BF16), pltpu.SemaphoreType.DMA((2, CHUNKS))],
        compiler_params=GRANT,
        cost_estimate=pl.CostEstimate(flops=4 * mine.shape[0] * w.shape[0] * w.shape[1], bytes_accessed=8 << 20, transcendentals=0),
    )(core, mine, other, w)


def split3(a):
    hi = a.astype(BF16)
    rest = a - hi.astype(F32)
    mid = rest.astype(BF16)
    return hi, mid, (rest - mid.astype(F32)).astype(BF16)


PARTS = 4


def read_kernel(info_ref, off_ref, mine_ref, other_ref, q_ref, cache_ref, out_ref, kv_ref, sems):
    blocks, half, width = mine_ref.shape
    span = kv_ref.shape[0]
    group = q_ref.shape[1]
    core, first = info_ref[0], info_ref[1]
    swap = core == 1
    piece = span // PARTS
    copies = []
    for b in range(blocks):
        a, o = mine_ref[b], other_ref[b]
        keys = jnp.where(swap, o, a)
        values = jnp.where(swap, a, o)
        base = 2 * half * b
        kv_ref[pl.ds(base, half)] = jnp.concatenate([keys[:, :HEAD_DIM], values[:, :HEAD_DIM]], axis=1)
        kv_ref[pl.ds(base + half, half)] = jnp.concatenate([keys[:, HEAD_DIM:], values[:, HEAD_DIM:]], axis=1)
        done = base + 2 * half
        if done % piece == 0:
            n = done // piece - 1
            copy = pltpu.make_async_copy(
                kv_ref.at[pl.ds(n * piece, piece)], cache_ref.at[0, 0, pl.ds(n * piece, piece)], sems.at[n]
            )
            copy.start()
            copies.append(copy)
    tiles = span // 128
    rows = 8
    q = jnp.concatenate([q_ref[0], jnp.zeros((group, width - HEAD_DIM), BF16)], axis=1)
    q = jnp.concatenate([q, jnp.zeros((rows - group, width), BF16)], axis=0)
    row = lax.broadcasted_iota(jnp.int32, (rows, 128), 0)
    off = jnp.zeros((rows, 128), F32)
    for g in range(group):
        off = jnp.where(row == g, off_ref[first + g], off)
    scores = lax.dot_general(q, kv_ref[...], (((1,), (1,)), ((), ())), preferred_element_type=F32)
    z = scores * (HEAD_DIM ** -0.5) + off[:, :1]
    stay = -(jnp.maximum(z, 0.0) + jnp.log1p(jnp.exp(-jnp.abs(z))))
    stacked = jnp.concatenate([stay[:, 128 * t : 128 * t + 128] for t in range(tiles)], axis=0)
    r = lax.broadcasted_iota(jnp.int32, (128, 128), 0)
    c = lax.broadcasted_iota(jnp.int32, (128, 128), 1)
    from_here = (r >= c).astype(F32).astype(BF16)
    suffix = None
    for part in split3(stacked):
        part = jnp.dot(part, from_here, preferred_element_type=F32)
        suffix = part if suffix is None else suffix + part
    later = jnp.zeros((rows, 1), F32)
    pieces = [None] * tiles
    for t in reversed(range(tiles)):
        own = suffix[rows * t : rows * t + rows]
        pieces[t] = own + later
        later = later + own[:, :1]
    weight = jnp.exp(z + jnp.concatenate(pieces, axis=1)).astype(BF16)
    out = jnp.dot(weight, kv_ref[...], preferred_element_type=F32)
    out_ref[0] = out[:group, HEAD_DIM:].astype(BF16)
    for copy in copies:
        copy.wait()


def read(info, off, mine, other, q):
    blocks, half, width = mine.shape
    span = 2 * blocks * half
    return pl.pallas_call(
        read_kernel,
        out_shape=(jax.ShapeDtypeStruct((1, 1, span, width), BF16), jax.ShapeDtypeStruct(q.shape, BF16)),
        in_specs=[SMEM, SMEM, VMEM, VMEM, VMEM],
        out_specs=(HBM, VMEM),
        scratch_shapes=[pltpu.VMEM((span, width), BF16), pltpu.SemaphoreType.DMA((PARTS,))],
        compiler_params=GRANT,
        cost_estimate=pl.CostEstimate(flops=32 * span * width, bytes_accessed=4 << 20, transcendentals=24 * span),
    )(info, off, mine, other, q)


def local(mixer_input, key_weight, content_projection_matrix, new_queries, head_stick_offset):
    seqs, block, width = mixer_input.shape
    depth, columns = key_weight.shape
    half = block // 2
    core = lax.axis_index("core").astype(jnp.int32)
    other = [(0, 1), (1, 0)]
    chips = lax.axis_size("x")
    weight = jnp.stack([key_weight, content_projection_matrix])
    weight = jnp.broadcast_to(weight, (chips, *weight.shape)).reshape(2 * chips, depth, columns)
    weight = lax.all_to_all(weight, ("x", "core"), 0, 0, tiled=True).reshape(2 * chips * depth, columns)
    rows = stage(mixer_input.reshape(seqs * block, width))
    their_rows = lax.ppermute(rows, "core", other)
    packed = project(core.reshape(1), rows, their_rows, weight, seqs, half)
    packed = lax.all_to_all(packed, "x", 0, 0, tiled=True)
    packed = packed.reshape(packed.shape[0] * 2 * seqs, half, 128)
    mine = lax.all_to_all(packed, ("z", "y"), 0, 0, tiled=True)
    theirs = lax.ppermute(mine, "core", other)
    first = (lax.axis_index("x") * 2 + core) * new_queries.shape[1]
    return read(jnp.stack([core, first]), head_stick_offset, mine, theirs, new_queries)


def solution(mesh):
    wide = Mesh(mesh.devices.reshape(2, 4, 8, 4, 2), ("gr", "z", "y", "x", "core"))
    sp, tp = ("z", "y"), ("x", "core")
    return jax.shard_map(
        local,
        mesh=wide,
        in_specs=(P(("gr", *tp), sp, None), P(tp, None), P(tp, None), P(("gr", *sp), tp, None), P()),
        out_specs=(P(("gr", *sp), tp, None, None), P(("gr", *sp), tp, None)),
        check_vma=False,
    )
```

```python
import jax
import jax.numpy as jnp
from jax import lax
from jax.experimental import pallas as pl
from jax.experimental.pallas import tpu as pltpu
from jax.sharding import Mesh, PartitionSpec as P


HEAD_DIM = 64
F32, BF16 = jnp.float32, jnp.bfloat16
SMEM = pl.BlockSpec(memory_space=pltpu.SMEM)
VMEM = pl.BlockSpec(memory_space=pltpu.VMEM)
HBM = pl.BlockSpec(memory_space=pltpu.HBM)
GRANT = pltpu.CompilerParams(vmem_limit_bytes=16 << 20)


def stage_kernel(x_ref, out_ref, sem):
    copy = pltpu.make_async_copy(x_ref, out_ref, sem)
    copy.start()
    copy.wait()


def stage(x):
    return pl.pallas_call(
        stage_kernel,
        out_shape=jax.ShapeDtypeStruct(x.shape, x.dtype),
        in_specs=[HBM],
        out_specs=VMEM,
        scratch_shapes=[pltpu.SemaphoreType.DMA],
        compiler_params=GRANT,
        cost_estimate=pl.CostEstimate(flops=1 << 30, bytes_accessed=6 << 20, transcendentals=0),
    )(x)


def spread_kernel(key_ref, value_ref, out_ref, held_ref, in_sems, out_sems):
    incoming = [pltpu.make_async_copy(ref, held_ref.at[n], in_sems.at[n]) for n, ref in enumerate((key_ref, value_ref))]
    for copy in incoming:
        copy.start()
    outgoing = []
    for n, copy in enumerate(incoming):
        copy.wait()
        for chip in range(out_ref.shape[0] // 2):
            out = pltpu.make_async_copy(held_ref.at[n], out_ref.at[2 * chip + n], out_sems.at[2 * chip + n])
            out.start()
            outgoing.append(out)
    for copy in outgoing:
        copy.wait()


def spread(key, value, chips):
    return pl.pallas_call(
        spread_kernel,
        out_shape=jax.ShapeDtypeStruct((2 * chips, *key.shape), key.dtype),
        in_specs=[HBM, HBM],
        out_specs=HBM,
        scratch_shapes=[
            pltpu.VMEM((2, *key.shape), key.dtype),
            pltpu.SemaphoreType.DMA((2,)),
            pltpu.SemaphoreType.DMA((2 * chips,)),
        ],
        cost_estimate=pl.CostEstimate(flops=1 << 20, bytes_accessed=2 << 20, transcendentals=0),
    )(key, value)


CHUNKS = 4


def project_kernel(core_ref, mine_ref, other_hbm, w_hbm, out_ref, other_ref, w_ref, sems):
    core = core_ref[0]
    heads, both, half, _ = out_ref.shape
    seqs = both // 2
    depth = w_ref.shape[0] // CHUNKS
    cuts = [pl.ds(k * depth, depth) for k in range(CHUNKS)]
    weights = [pltpu.make_async_copy(w_hbm.at[c], w_ref.at[c], sems.at[0, k]) for k, c in enumerate(cuts)]
    others = [pltpu.make_async_copy(other_hbm.at[:, c], other_ref.at[:, c], sems.at[1, k]) for k, c in enumerate(cuts)]
    for copy in weights:
        copy.start()
    for copy in weights:
        copy.wait()
    for copy in others:
        copy.start()
    for ref, which, copies in ((mine_ref, core, None), (other_ref, 1 - core, others)):
        rows = None
        for k, c in enumerate(cuts):
            if copies is not None:
                copies[k].wait()
            part = jnp.dot(ref[:, c], w_ref[c], preferred_element_type=F32)
            rows = part if rows is None else rows + part
        for i in range(seqs):
            for h in range(heads):
                part = rows[2 * half * i : 2 * half * (i + 1), HEAD_DIM * h : HEAD_DIM * h + HEAD_DIM]
                out_ref[h, which * seqs + i] = jnp.concatenate([part[:half], part[half:]], axis=1).astype(BF16)


def project(core, mine, other, w, seqs, half):
    heads = w.shape[1] // HEAD_DIM
    return pl.pallas_call(
        project_kernel,
        out_shape=jax.ShapeDtypeStruct((heads, 2 * seqs, half, 128), BF16),
        in_specs=[SMEM, VMEM, HBM, HBM],
        out_specs=VMEM,
        scratch_shapes=[pltpu.VMEM(other.shape, BF16), pltpu.VMEM(w.shape, BF16), pltpu.SemaphoreType.DMA((2, CHUNKS))],
        compiler_params=GRANT,
        cost_estimate=pl.CostEstimate(flops=4 * mine.shape[0] * w.shape[0] * w.shape[1], bytes_accessed=8 << 20, transcendentals=0),
    )(core, mine, other, w)


def split3(a):
    hi = a.astype(BF16)
    rest = a - hi.astype(F32)
    mid = rest.astype(BF16)
    return hi, mid, (rest - mid.astype(F32)).astype(BF16)


PARTS = 4


def read_kernel(info_ref, off_ref, mine_ref, other_ref, q_ref, cache_ref, out_ref, kv_ref, sems):
    blocks, half, width = mine_ref.shape
    span = kv_ref.shape[0]
    group = q_ref.shape[1]
    core, first = info_ref[0], info_ref[1]
    swap = core == 1
    piece = span // PARTS
    copies = []
    for b in range(blocks):
        a, o = mine_ref[b], other_ref[b]
        keys = jnp.where(swap, o, a)
        values = jnp.where(swap, a, o)
        base = 2 * half * b
        kv_ref[pl.ds(base, half)] = jnp.concatenate([keys[:, :HEAD_DIM], values[:, :HEAD_DIM]], axis=1)
        kv_ref[pl.ds(base + half, half)] = jnp.concatenate([keys[:, HEAD_DIM:], values[:, HEAD_DIM:]], axis=1)
        done = base + 2 * half
        if done % piece == 0:
            n = done // piece - 1
            copy = pltpu.make_async_copy(
                kv_ref.at[pl.ds(n * piece, piece)], cache_ref.at[0, 0, pl.ds(n * piece, piece)], sems.at[n]
            )
            copy.start()
            copies.append(copy)
    tiles = span // 128
    rows = 8
    q = jnp.concatenate([q_ref[0], jnp.zeros((group, width - HEAD_DIM), BF16)], axis=1)
    q = jnp.concatenate([q, jnp.zeros((rows - group, width), BF16)], axis=0)
    row = lax.broadcasted_iota(jnp.int32, (rows, 128), 0)
    off = jnp.zeros((rows, 128), F32)
    for g in range(group):
        off = jnp.where(row == g, off_ref[first + g], off)
    scores = lax.dot_general(q, kv_ref[...], (((1,), (1,)), ((), ())), preferred_element_type=F32)
    z = scores * (HEAD_DIM ** -0.5) + off[:, :1]
    stay = -(jnp.maximum(z, 0.0) + jnp.log1p(jnp.exp(-jnp.abs(z))))
    stacked = jnp.concatenate([stay[:, 128 * t : 128 * t + 128] for t in range(tiles)], axis=0)
    r = lax.broadcasted_iota(jnp.int32, (128, 128), 0)
    c = lax.broadcasted_iota(jnp.int32, (128, 128), 1)
    from_here = (r >= c).astype(F32).astype(BF16)
    suffix = None
    for part in split3(stacked):
        part = jnp.dot(part, from_here, preferred_element_type=F32)
        suffix = part if suffix is None else suffix + part
    later = jnp.zeros((rows, 1), F32)
    pieces = [None] * tiles
    for t in reversed(range(tiles)):
        own = suffix[rows * t : rows * t + rows]
        pieces[t] = own + later
        later = later + own[:, :1]
    weight = jnp.exp(z + jnp.concatenate(pieces, axis=1)).astype(BF16)
    out = jnp.dot(weight, kv_ref[...], preferred_element_type=F32)
    out_ref[0] = out[:group, HEAD_DIM:].astype(BF16)
    for copy in copies:
        copy.wait()


def read(info, off, mine, other, q):
    blocks, half, width = mine.shape
    span = 2 * blocks * half
    return pl.pallas_call(
        read_kernel,
        out_shape=(jax.ShapeDtypeStruct((1, 1, span, width), BF16), jax.ShapeDtypeStruct(q.shape, BF16)),
        in_specs=[SMEM, SMEM, VMEM, VMEM, VMEM],
        out_specs=(HBM, VMEM),
        scratch_shapes=[pltpu.VMEM((span, width), BF16), pltpu.SemaphoreType.DMA((PARTS,))],
        compiler_params=GRANT,
        cost_estimate=pl.CostEstimate(flops=32 * span * width, bytes_accessed=4 << 20, transcendentals=24 * span),
    )(info, off, mine, other, q)


def local(mixer_input, key_weight, content_projection_matrix, new_queries, head_stick_offset):
    seqs, block, width = mixer_input.shape
    depth, columns = key_weight.shape
    half = block // 2
    core = lax.axis_index("core").astype(jnp.int32)
    other = [(0, 1), (1, 0)]
    chips = lax.axis_size("x")
    weight = spread(key_weight, content_projection_matrix, chips)
    weight = lax.all_to_all(weight, ("x", "core"), 0, 0, tiled=True).reshape(2 * chips * depth, columns)
    rows = stage(mixer_input.reshape(seqs * block, width))
    their_rows = lax.ppermute(rows, "core", other)
    packed = project(core.reshape(1), rows, their_rows, weight, seqs, half)
    packed = lax.all_to_all(packed, "x", 0, 0, tiled=True)
    packed = packed.reshape(packed.shape[0] * 2 * seqs, half, 128)
    mine = lax.all_to_all(packed, ("z", "y"), 0, 0, tiled=True)
    theirs = lax.ppermute(mine, "core", other)
    first = (lax.axis_index("x") * 2 + core) * new_queries.shape[1]
    return read(jnp.stack([core, first]), head_stick_offset, mine, theirs, new_queries)


def solution(mesh):
    wide = Mesh(mesh.devices.reshape(2, 4, 8, 4, 2), ("gr", "z", "y", "x", "core"))
    sp, tp = ("z", "y"), ("x", "core")
    return jax.shard_map(
        local,
        mesh=wide,
        in_specs=(P(("gr", *tp), sp, None), P(tp, None), P(tp, None), P(("gr", *sp), tp, None), P()),
        out_specs=(P(("gr", *sp), tp, None, None), P(("gr", *sp), tp, None)),
        check_vma=False,
    )
```

```python
import jax
import jax.numpy as jnp
from jax import lax
from jax.experimental import pallas as pl
from jax.experimental.pallas import tpu as pltpu
from jax.sharding import Mesh, PartitionSpec as P

HEAD_DIM = 64
F32, BF16 = jnp.float32, jnp.bfloat16
SMEM = pl.BlockSpec(memory_space=pltpu.SMEM)
VMEM = pl.BlockSpec(memory_space=pltpu.VMEM)
HBM = pl.BlockSpec(memory_space=pltpu.HBM)
GRANT = pltpu.CompilerParams(vmem_limit_bytes=16 << 20)


def project_kernel(mine_ref, other_ref, w_ref, out_ref):
    core = lax.axis_index("core")
    heads, both, half, _ = out_ref.shape
    seqs = both // 2
    for ref, which in ((mine_ref, core), (other_ref, 1 - core)):
        rows = jnp.dot(ref[...], w_ref[...], preferred_element_type=F32)
        for i in range(seqs):
            for h in range(heads):
                part = rows[2 * half * i : 2 * half * (i + 1), HEAD_DIM * h : HEAD_DIM * h + HEAD_DIM]
                out_ref[h, which * seqs + i] = jnp.concatenate([part[:half], part[half:]], axis=1).astype(BF16)


def project(mine, other, w, seqs, half):
    heads = w.shape[1] // HEAD_DIM
    return pl.pallas_call(
        project_kernel,
        out_shape=jax.ShapeDtypeStruct((heads, 2 * seqs, half, 128), BF16),
        in_specs=[VMEM, VMEM, VMEM],
        out_specs=VMEM,
        compiler_params=GRANT,
        cost_estimate=pl.CostEstimate(flops=4 * mine.shape[0] * w.shape[0] * w.shape[1], bytes_accessed=8 << 20, transcendentals=0),
    )(mine, other, w)


def split3(a):
    hi = a.astype(BF16)
    rest = a - hi.astype(F32)
    mid = rest.astype(BF16)
    return hi, mid, (rest - mid.astype(F32)).astype(BF16)


PARTS = 4


def read_kernel(off_ref, mine_ref, other_ref, q_ref, cache_ref, out_ref, kv_ref, sems):
    blocks, half, width = mine_ref.shape
    span = kv_ref.shape[0]
    group = q_ref.shape[1]
    core = lax.axis_index("core")
    first = (lax.axis_index("x") * 2 + core) * group
    swap = core == 1
    piece = span // PARTS
    copies = []
    for b in range(blocks):
        a, o = mine_ref[b], other_ref[b]
        keys = jnp.where(swap, o, a)
        values = jnp.where(swap, a, o)
        base = 2 * half * b
        kv_ref[pl.ds(base, half)] = jnp.concatenate([keys[:, :HEAD_DIM], values[:, :HEAD_DIM]], axis=1)
        kv_ref[pl.ds(base + half, half)] = jnp.concatenate([keys[:, HEAD_DIM:], values[:, HEAD_DIM:]], axis=1)
        done = base + 2 * half
        if done % piece == 0:
            n = done // piece - 1
            copy = pltpu.make_async_copy(
                kv_ref.at[pl.ds(n * piece, piece)], cache_ref.at[0, 0, pl.ds(n * piece, piece)], sems.at[n]
            )
            copy.start()
            copies.append(copy)
    tiles = span // 128
    rows = 8
    q = jnp.concatenate([q_ref[0], jnp.zeros((group, width - HEAD_DIM), BF16)], axis=1)
    q = jnp.concatenate([q, jnp.zeros((rows - group, width), BF16)], axis=0)
    row = lax.broadcasted_iota(jnp.int32, (rows, 128), 0)
    off = jnp.zeros((rows, 128), F32)
    for g in range(group):
        off = jnp.where(row == g, off_ref[first + g], off)
    scores = lax.dot_general(q, kv_ref[...], (((1,), (1,)), ((), ())), preferred_element_type=F32)
    z = scores * (HEAD_DIM ** -0.5) + off[:, :1]
    stay = -(jnp.maximum(z, 0.0) + jnp.log1p(jnp.exp(-jnp.abs(z))))
    stacked = jnp.concatenate([stay[:, 128 * t : 128 * t + 128] for t in range(tiles)], axis=0)
    r = lax.broadcasted_iota(jnp.int32, (128, 128), 0)
    c = lax.broadcasted_iota(jnp.int32, (128, 128), 1)
    from_here = (r >= c).astype(F32).astype(BF16)
    suffix = None
    for part in split3(stacked):
        part = jnp.dot(part, from_here, preferred_element_type=F32)
        suffix = part if suffix is None else suffix + part
    later = jnp.zeros((rows, 1), F32)
    pieces = [None] * tiles
    for t in reversed(range(tiles)):
        own = suffix[rows * t : rows * t + rows]
        pieces[t] = own + later
        later = later + own[:, :1]
    weight = jnp.exp(z + jnp.concatenate(pieces, axis=1)).astype(BF16)
    out = jnp.dot(weight, kv_ref[...], preferred_element_type=F32)
    out_ref[0] = out[:group, HEAD_DIM:].astype(BF16)
    for copy in copies:
        copy.wait()


def read(off, mine, other, q):
    blocks, half, width = mine.shape
    span = 2 * blocks * half
    group = q.shape[1]
    return pl.pallas_call(
        read_kernel,
        out_shape=(jax.ShapeDtypeStruct((1, 1, span, width), BF16), jax.ShapeDtypeStruct(q.shape, BF16)),
        in_specs=[SMEM, VMEM, VMEM, VMEM],
        out_specs=(HBM, VMEM),
        scratch_shapes=[pltpu.VMEM((span, width), BF16), pltpu.SemaphoreType.DMA((PARTS,))],
        compiler_params=GRANT,
        cost_estimate=pl.CostEstimate(flops=32 * span * width, bytes_accessed=4 << 20, transcendentals=24 * span),
    )(off, mine, other, q)


def local(mixer_input, key_weight, content_projection_matrix, new_queries, head_stick_offset):
    seqs, block, width = mixer_input.shape
    depth, columns = key_weight.shape
    half = block // 2
    other = [(0, 1), (1, 0)]
    chips = lax.axis_size("x")
    rows = mixer_input.reshape(seqs * block, width)
    their_rows = lax.ppermute(rows, "core", other)
    weight = jnp.stack([key_weight, content_projection_matrix])
    weight = jnp.broadcast_to(weight, (chips, *weight.shape)).reshape(2 * chips, depth, columns)
    weight = lax.all_to_all(weight, ("x", "core"), 0, 0, tiled=True).reshape(2 * chips * depth, columns)
    packed = project(rows, their_rows, weight, seqs, half)
    packed = lax.all_to_all(packed, "x", 0, 0, tiled=True)
    packed = packed.reshape(packed.shape[0] * 2 * seqs, half, 128)
    mine = lax.all_to_all(packed, ("z", "y"), 0, 0, tiled=True)
    theirs = lax.ppermute(mine, "core", other)
    return read(head_stick_offset, mine, theirs, new_queries)


def solution(mesh):
    wide = Mesh(mesh.devices.reshape(2, 4, 8, 4, 2), ("gr", "z", "y", "x", "core"))
    sp, tp = ("z", "y"), ("x", "core")
    return jax.shard_map(
        local,
        mesh=wide,
        in_specs=(P(("gr", *tp), sp, None), P(tp, None), P(tp, None), P(("gr", *sp), tp, None), P()),
        out_specs=(P(("gr", *sp), tp, None, None), P(("gr", *sp), tp, None)),
        check_vma=False,
    )
```

```python
import jax
import jax.numpy as jnp
import numpy as np
from jax import lax
from jax.experimental import pallas as pl
from jax.experimental.pallas import tpu as pltpu
from jax.sharding import Mesh, PartitionSpec as P

HEAD_DIM = 64
F32, BF16 = jnp.float32, jnp.bfloat16
SMEM = pl.BlockSpec(memory_space=pltpu.SMEM)
VMEM = pl.BlockSpec(memory_space=pltpu.VMEM)
HBM = pl.BlockSpec(memory_space=pltpu.HBM)
GRANT = pltpu.CompilerParams(vmem_limit_bytes=16 << 20)


def project_kernel(mine_ref, other_ref, w_ref, out_ref):
    core = lax.axis_index("core")
    heads, both, half, _ = out_ref.shape
    seqs = both // 2
    depth = w_ref.shape[1]
    for ref, which in ((mine_ref, core), (other_ref, 1 - core)):
        rows = None
        for n, shard in enumerate(SHARD_OF):
            part = jnp.dot(ref[:, depth * shard : depth * (shard + 1)], w_ref[n], preferred_element_type=F32)
            rows = part if rows is None else rows + part
        for i in range(seqs):
            for h in range(heads):
                part = rows[2 * half * i : 2 * half * (i + 1), HEAD_DIM * h : HEAD_DIM * h + HEAD_DIM]
                out_ref[CHIP_AT[h], which * seqs + i] = jnp.concatenate([part[:half], part[half:]], axis=1).astype(BF16)


def project(mine, other, w, seqs, half):
    heads = w.shape[2] // HEAD_DIM
    return pl.pallas_call(
        project_kernel,
        out_shape=jax.ShapeDtypeStruct((heads, 2 * seqs, half, 128), BF16),
        in_specs=[VMEM, VMEM, VMEM],
        out_specs=VMEM,
        compiler_params=GRANT,
        cost_estimate=pl.CostEstimate(flops=4 * mine.shape[0] * mine.shape[1] * w.shape[2], bytes_accessed=8 << 20, transcendentals=0),
    )(mine, other, w)


def split3(a):
    hi = a.astype(BF16)
    rest = a - hi.astype(F32)
    mid = rest.astype(BF16)
    return hi, mid, (rest - mid.astype(F32)).astype(BF16)


PARTS = 4
BITS = ("z1", "z0", "y2", "y1", "y0")
LINE = ("x1", "x0")
WEIGHT_ORDER = ("x0", "core", "x1")
CHIP_ORDER = ("x0", "x1")
ORDER = ("y2", "z1", "y1", "z0", "y0")


def places(names, order):
    return np.arange(2 ** len(names)).reshape([2] * len(names)).transpose([order.index(n) for n in names]).ravel().tolist()


SHARD_OF = places(WEIGHT_ORDER, (*LINE, "core"))
CHIP_AT = places(LINE, CHIP_ORDER)
BLOCK_AT = places(BITS, ORDER)


def read_kernel(off_ref, mine_ref, other_ref, q_ref, cache_ref, out_ref, kv_ref, sems):
    blocks, half, width = mine_ref.shape
    span = kv_ref.shape[0]
    group = q_ref.shape[1]
    core = lax.axis_index("core")
    first = ((lax.axis_index("x1") * 2 + lax.axis_index("x0")) * 2 + core) * group
    swap = core == 1
    piece = span // PARTS
    copies = []
    for b, n in enumerate(BLOCK_AT):
        a, o = mine_ref[n], other_ref[n]
        keys = jnp.where(swap, o, a)
        values = jnp.where(swap, a, o)
        base = 2 * half * b
        kv_ref[pl.ds(base, half)] = jnp.concatenate([keys[:, :HEAD_DIM], values[:, :HEAD_DIM]], axis=1)
        kv_ref[pl.ds(base + half, half)] = jnp.concatenate([keys[:, HEAD_DIM:], values[:, HEAD_DIM:]], axis=1)
        done = base + 2 * half
        if done % piece == 0:
            n = done // piece - 1
            copy = pltpu.make_async_copy(
                kv_ref.at[pl.ds(n * piece, piece)], cache_ref.at[0, 0, pl.ds(n * piece, piece)], sems.at[n]
            )
            copy.start()
            copies.append(copy)
    tiles = span // 128
    rows = 8
    q = jnp.concatenate([q_ref[0], jnp.zeros((group, width - HEAD_DIM), BF16)], axis=1)
    q = jnp.concatenate([q, jnp.zeros((rows - group, width), BF16)], axis=0)
    row = lax.broadcasted_iota(jnp.int32, (rows, 128), 0)
    off = jnp.zeros((rows, 128), F32)
    for g in range(group):
        off = jnp.where(row == g, off_ref[first + g], off)
    scores = lax.dot_general(q, kv_ref[...], (((1,), (1,)), ((), ())), preferred_element_type=F32)
    z = scores * (HEAD_DIM ** -0.5) + off[:, :1]
    stay = -(jnp.maximum(z, 0.0) + jnp.log1p(jnp.exp(-jnp.abs(z))))
    stacked = jnp.concatenate([stay[:, 128 * t : 128 * t + 128] for t in range(tiles)], axis=0)
    r = lax.broadcasted_iota(jnp.int32, (128, 128), 0)
    c = lax.broadcasted_iota(jnp.int32, (128, 128), 1)
    from_here = (r >= c).astype(F32).astype(BF16)
    suffix = None
    for part in split3(stacked):
        part = jnp.dot(part, from_here, preferred_element_type=F32)
        suffix = part if suffix is None else suffix + part
    later = jnp.zeros((rows, 1), F32)
    pieces = [None] * tiles
    for t in reversed(range(tiles)):
        own = suffix[rows * t : rows * t + rows]
        pieces[t] = own + later
        later = later + own[:, :1]
    weight = jnp.exp(z + jnp.concatenate(pieces, axis=1)).astype(BF16)
    out = jnp.dot(weight, kv_ref[...], preferred_element_type=F32)
    out_ref[0] = out[:group, HEAD_DIM:].astype(BF16)
    for copy in copies:
        copy.wait()


def read(off, mine, other, q):
    blocks, half, width = mine.shape
    span = 2 * blocks * half
    group = q.shape[1]
    return pl.pallas_call(
        read_kernel,
        out_shape=(jax.ShapeDtypeStruct((1, 1, span, width), BF16), jax.ShapeDtypeStruct(q.shape, BF16)),
        in_specs=[SMEM, VMEM, VMEM, VMEM],
        out_specs=(HBM, VMEM),
        scratch_shapes=[pltpu.VMEM((span, width), BF16), pltpu.SemaphoreType.DMA((PARTS,))],
        compiler_params=GRANT,
        cost_estimate=pl.CostEstimate(flops=32 * span * width, bytes_accessed=4 << 20, transcendentals=24 * span),
    )(off, mine, other, q)


def local(mixer_input, key_weight, content_projection_matrix, new_queries, head_stick_offset):
    seqs, block, width = mixer_input.shape
    depth, columns = key_weight.shape
    half = block // 2
    other = [(0, 1), (1, 0)]
    rows = mixer_input.reshape(seqs * block, width)
    their_rows = lax.ppermute(rows, "core", other)
    pair = jnp.stack([key_weight, content_projection_matrix])
    shape = [2 if name == "core" else 1 for name in WEIGHT_ORDER]
    weight = jnp.broadcast_to(pair.reshape(*shape, depth, columns), (2, 2, 2, depth, columns)).reshape(8, depth, columns)
    weight = lax.all_to_all(weight, WEIGHT_ORDER, 0, 0, tiled=True)
    packed = project(rows, their_rows, weight, seqs, half)
    packed = lax.all_to_all(packed, CHIP_ORDER, 0, 0, tiled=True)
    held = (*(name.replace("x", "z") for name in CHIP_ORDER), "y2", "y1", "y0")
    packed = packed.reshape(2, 2, 2, 2, 2, half, 128).transpose(*(held.index(n) for n in ORDER), 5, 6).reshape(-1, half, 128)
    mine = lax.all_to_all(packed, ORDER, 0, 0, tiled=True)
    theirs = lax.ppermute(mine, "core", other)
    return read(head_stick_offset, mine, theirs, new_queries)


def solution(mesh):
    wide = Mesh(mesh.devices.reshape([2] * 9), ("gr", *BITS, *LINE, "core"))
    sp, tp = BITS, (*LINE, "core")
    return jax.shard_map(
        local,
        mesh=wide,
        in_specs=(P(("gr", *tp), sp, None), P(tp, None), P(tp, None), P(("gr", *sp), tp, None), P()),
        out_specs=(P(("gr", *sp), tp, None, None), P(("gr", *sp), tp, None)),
        check_vma=False,
    )
```

```python
import jax
import jax.numpy as jnp
import numpy as np
from jax import lax
from jax.experimental import pallas as pl
from jax.experimental.pallas import tpu as pltpu
from jax.sharding import Mesh, PartitionSpec as P

HEAD_DIM = 64
F32, BF16 = jnp.float32, jnp.bfloat16
SMEM = pl.BlockSpec(memory_space=pltpu.SMEM)
VMEM = pl.BlockSpec(memory_space=pltpu.VMEM)
HBM = pl.BlockSpec(memory_space=pltpu.HBM)
GRANT = pltpu.CompilerParams(vmem_limit_bytes=16 << 20)


def project_kernel(mine_ref, other_ref, w_ref, out_ref):
    core = lax.axis_index("core")
    heads, both, half, _ = out_ref.shape
    seqs = both // 2
    depth = w_ref.shape[1]
    for ref, which in ((mine_ref, core), (other_ref, 1 - core)):
        rows = None
        for n, shard in enumerate(SHARD_OF):
            part = jnp.dot(ref[:, depth * shard : depth * (shard + 1)], w_ref[n], preferred_element_type=F32)
            rows = part if rows is None else rows + part
        for i in range(seqs):
            for h in range(heads):
                part = rows[2 * half * i : 2 * half * (i + 1), HEAD_DIM * h : HEAD_DIM * h + HEAD_DIM]
                out_ref[CHIP_AT[h], which * seqs + i] = jnp.concatenate([part[:half], part[half:]], axis=1).astype(BF16)


def project(mine, other, w, seqs, half):
    heads = w.shape[2] // HEAD_DIM
    return pl.pallas_call(
        project_kernel,
        out_shape=jax.ShapeDtypeStruct((heads, 2 * seqs, half, 128), BF16),
        in_specs=[VMEM, VMEM, VMEM],
        out_specs=VMEM,
        compiler_params=GRANT,
        cost_estimate=pl.CostEstimate(flops=4 * mine.shape[0] * mine.shape[1] * w.shape[2], bytes_accessed=8 << 20, transcendentals=0),
    )(mine, other, w)


def split3(a):
    hi = a.astype(BF16)
    rest = a - hi.astype(F32)
    mid = rest.astype(BF16)
    return hi, mid, (rest - mid.astype(F32)).astype(BF16)


PARTS = 4
BITS = ("z1", "z0", "y2", "y1", "y0")
LINE = ("x1", "x0")
WEIGHT_ORDER = ("x0", "core", "x1")
CHIP_ORDER = ("x0", "x1")
ORDER = ("y0", "y1", "z1", "z0", "y2")


def places(names, order):
    return np.arange(2 ** len(names)).reshape([2] * len(names)).transpose([order.index(n) for n in names]).ravel().tolist()


SHARD_OF = places(WEIGHT_ORDER, (*LINE, "core"))
CHIP_AT = places(LINE, CHIP_ORDER)
BLOCK_AT = places(BITS, ORDER)


def read_kernel(off_ref, mine_ref, other_ref, q_ref, cache_ref, out_ref, kv_ref, sems):
    blocks, half, width = mine_ref.shape
    span = kv_ref.shape[0]
    group = q_ref.shape[1]
    core = lax.axis_index("core")
    first = ((lax.axis_index("x1") * 2 + lax.axis_index("x0")) * 2 + core) * group
    swap = core == 1
    piece = span // PARTS
    copies = []
    for b, n in enumerate(BLOCK_AT):
        a, o = mine_ref[n], other_ref[n]
        keys = jnp.where(swap, o, a)
        values = jnp.where(swap, a, o)
        base = 2 * half * b
        kv_ref[pl.ds(base, half)] = jnp.concatenate([keys[:, :HEAD_DIM], values[:, :HEAD_DIM]], axis=1)
        kv_ref[pl.ds(base + half, half)] = jnp.concatenate([keys[:, HEAD_DIM:], values[:, HEAD_DIM:]], axis=1)
        done = base + 2 * half
        if done % piece == 0:
            n = done // piece - 1
            copy = pltpu.make_async_copy(
                kv_ref.at[pl.ds(n * piece, piece)], cache_ref.at[0, 0, pl.ds(n * piece, piece)], sems.at[n]
            )
            copy.start()
            copies.append(copy)
    tiles = span // 128
    rows = 8
    q = jnp.concatenate([q_ref[0], jnp.zeros((group, width - HEAD_DIM), BF16)], axis=1)
    q = jnp.concatenate([q, jnp.zeros((rows - group, width), BF16)], axis=0)
    row = lax.broadcasted_iota(jnp.int32, (rows, 128), 0)
    off = jnp.zeros((rows, 128), F32)
    for g in range(group):
        off = jnp.where(row == g, off_ref[first + g], off)
    scores = lax.dot_general(q, kv_ref[...], (((1,), (1,)), ((), ())), preferred_element_type=F32)
    z = scores * (HEAD_DIM ** -0.5) + off[:, :1]
    stay = -(jnp.maximum(z, 0.0) + jnp.log1p(jnp.exp(-jnp.abs(z))))
    stacked = jnp.concatenate([stay[:, 128 * t : 128 * t + 128] for t in range(tiles)], axis=0)
    r = lax.broadcasted_iota(jnp.int32, (128, 128), 0)
    c = lax.broadcasted_iota(jnp.int32, (128, 128), 1)
    from_here = (r >= c).astype(F32).astype(BF16)
    suffix = None
    for part in split3(stacked):
        part = jnp.dot(part, from_here, preferred_element_type=F32)
        suffix = part if suffix is None else suffix + part
    later = jnp.zeros((rows, 1), F32)
    pieces = [None] * tiles
    for t in reversed(range(tiles)):
        own = suffix[rows * t : rows * t + rows]
        pieces[t] = own + later
        later = later + own[:, :1]
    weight = jnp.exp(z + jnp.concatenate(pieces, axis=1)).astype(BF16)
    out = jnp.dot(weight, kv_ref[...], preferred_element_type=F32)
    out_ref[0] = out[:group, HEAD_DIM:].astype(BF16)
    for copy in copies:
        copy.wait()


def read(off, mine, other, q):
    blocks, half, width = mine.shape
    span = 2 * blocks * half
    group = q.shape[1]
    return pl.pallas_call(
        read_kernel,
        out_shape=(jax.ShapeDtypeStruct((1, 1, span, width), BF16), jax.ShapeDtypeStruct(q.shape, BF16)),
        in_specs=[SMEM, VMEM, VMEM, VMEM],
        out_specs=(HBM, VMEM),
        scratch_shapes=[pltpu.VMEM((span, width), BF16), pltpu.SemaphoreType.DMA((PARTS,))],
        compiler_params=GRANT,
        cost_estimate=pl.CostEstimate(flops=32 * span * width, bytes_accessed=4 << 20, transcendentals=24 * span),
    )(off, mine, other, q)


def local(mixer_input, key_weight, content_projection_matrix, new_queries, head_stick_offset):
    seqs, block, width = mixer_input.shape
    depth, columns = key_weight.shape
    half = block // 2
    other = [(0, 1), (1, 0)]
    rows = mixer_input.reshape(seqs * block, width)
    their_rows = lax.ppermute(rows, "core", other)
    pair = jnp.stack([key_weight, content_projection_matrix])
    shape = [2 if name == "core" else 1 for name in WEIGHT_ORDER]
    weight = jnp.broadcast_to(pair.reshape(*shape, depth, columns), (2, 2, 2, depth, columns)).reshape(8, depth, columns)
    weight = lax.all_to_all(weight, WEIGHT_ORDER, 0, 0, tiled=True)
    packed = project(rows, their_rows, weight, seqs, half)
    packed = lax.all_to_all(packed, CHIP_ORDER, 0, 0, tiled=True)
    held = (*(name.replace("x", "z") for name in CHIP_ORDER), "y2", "y1", "y0")
    packed = packed.reshape(2, 2, 2, 2, 2, half, 128).transpose(*(held.index(n) for n in ORDER), 5, 6).reshape(-1, half, 128)
    mine = lax.all_to_all(packed, ORDER, 0, 0, tiled=True)
    theirs = lax.ppermute(mine, "core", other)
    return read(head_stick_offset, mine, theirs, new_queries)


def solution(mesh):
    wide = Mesh(mesh.devices.reshape([2] * 9), ("gr", *BITS, *LINE, "core"))
    sp, tp = BITS, (*LINE, "core")
    return jax.shard_map(
        local,
        mesh=wide,
        in_specs=(P(("gr", *tp), sp, None), P(tp, None), P(tp, None), P(("gr", *sp), tp, None), P()),
        out_specs=(P(("gr", *sp), tp, None, None), P(("gr", *sp), tp, None)),
        check_vma=False,
    )
```

```python
import jax
import jax.numpy as jnp
import numpy as np
from jax import lax
from jax.experimental import pallas as pl
from jax.experimental.pallas import tpu as pltpu
from jax.sharding import Mesh, PartitionSpec as P

HEAD_DIM = 64
F32, BF16 = jnp.float32, jnp.bfloat16
SMEM = pl.BlockSpec(memory_space=pltpu.SMEM)
VMEM = pl.BlockSpec(memory_space=pltpu.VMEM)
HBM = pl.BlockSpec(memory_space=pltpu.HBM)
GRANT = pltpu.CompilerParams(vmem_limit_bytes=16 << 20)


def project_kernel(mine_ref, other_ref, w_ref, out_ref):
    core = lax.axis_index("core")
    heads, both, half, _ = out_ref.shape
    seqs = both // 2
    depth = w_ref.shape[1]
    for ref, which in ((mine_ref, core), (other_ref, 1 - core)):
        rows = None
        for n, shard in enumerate(SHARD_OF):
            part = jnp.dot(ref[:, depth * shard : depth * (shard + 1)], w_ref[n], preferred_element_type=F32)
            rows = part if rows is None else rows + part
        for i in range(seqs):
            for h in range(heads):
                part = rows[2 * half * i : 2 * half * (i + 1), HEAD_DIM * h : HEAD_DIM * h + HEAD_DIM]
                out_ref[CHIP_AT[h], which * seqs + i] = jnp.concatenate([part[:half], part[half:]], axis=1).astype(BF16)


def project(mine, other, w, seqs, half):
    heads = w.shape[2] // HEAD_DIM
    return pl.pallas_call(
        project_kernel,
        out_shape=jax.ShapeDtypeStruct((heads, 2 * seqs, half, 128), BF16),
        in_specs=[VMEM, VMEM, VMEM],
        out_specs=VMEM,
        compiler_params=GRANT,
        cost_estimate=pl.CostEstimate(flops=4 * mine.shape[0] * mine.shape[1] * w.shape[2], bytes_accessed=8 << 20, transcendentals=0),
    )(mine, other, w)


def split3(a):
    hi = a.astype(BF16)
    rest = a - hi.astype(F32)
    mid = rest.astype(BF16)
    return hi, mid, (rest - mid.astype(F32)).astype(BF16)


PARTS = 4
BITS = ("z1", "z0", "y2", "y1", "y0")
LINE = ("x1", "x0")
WEIGHT_ORDER = ("core", "x0", "x1")
CHIP_ORDER = ("x0", "x1")
ORDER = ("y0", "y1", "z1", "z0", "y2")


def places(names, order):
    return np.arange(2 ** len(names)).reshape([2] * len(names)).transpose([order.index(n) for n in names]).ravel().tolist()


SHARD_OF = places(WEIGHT_ORDER, (*LINE, "core"))
CHIP_AT = places(LINE, CHIP_ORDER)
BLOCK_AT = places(BITS, ORDER)


def read_kernel(off_ref, mine_ref, other_ref, q_ref, cache_ref, out_ref, kv_ref, sems):
    blocks, half, width = mine_ref.shape
    span = kv_ref.shape[0]
    group = q_ref.shape[1]
    core = lax.axis_index("core")
    first = ((lax.axis_index("x1") * 2 + lax.axis_index("x0")) * 2 + core) * group
    swap = core == 1
    piece = span // PARTS
    copies = []
    for b, n in enumerate(BLOCK_AT):
        a, o = mine_ref[n], other_ref[n]
        keys = jnp.where(swap, o, a)
        values = jnp.where(swap, a, o)
        base = 2 * half * b
        kv_ref[pl.ds(base, half)] = jnp.concatenate([keys[:, :HEAD_DIM], values[:, :HEAD_DIM]], axis=1)
        kv_ref[pl.ds(base + half, half)] = jnp.concatenate([keys[:, HEAD_DIM:], values[:, HEAD_DIM:]], axis=1)
        done = base + 2 * half
        if done % piece == 0:
            n = done // piece - 1
            copy = pltpu.make_async_copy(
                kv_ref.at[pl.ds(n * piece, piece)], cache_ref.at[0, 0, pl.ds(n * piece, piece)], sems.at[n]
            )
            copy.start()
            copies.append(copy)
    tiles = span // 128
    rows = 8
    q = jnp.concatenate([q_ref[0], jnp.zeros((group, width - HEAD_DIM), BF16)], axis=1)
    q = jnp.concatenate([q, jnp.zeros((rows - group, width), BF16)], axis=0)
    row = lax.broadcasted_iota(jnp.int32, (rows, 128), 0)
    off = jnp.zeros((rows, 128), F32)
    for g in range(group):
        off = jnp.where(row == g, off_ref[first + g], off)
    scores = lax.dot_general(q, kv_ref[...], (((1,), (1,)), ((), ())), preferred_element_type=F32)
    z = scores * (HEAD_DIM ** -0.5) + off[:, :1]
    stay = -(jnp.maximum(z, 0.0) + jnp.log1p(jnp.exp(-jnp.abs(z))))
    stacked = jnp.concatenate([stay[:, 128 * t : 128 * t + 128] for t in range(tiles)], axis=0)
    r = lax.broadcasted_iota(jnp.int32, (128, 128), 0)
    c = lax.broadcasted_iota(jnp.int32, (128, 128), 1)
    from_here = (r >= c).astype(F32).astype(BF16)
    suffix = None
    for part in split3(stacked):
        part = jnp.dot(part, from_here, preferred_element_type=F32)
        suffix = part if suffix is None else suffix + part
    later = jnp.zeros((rows, 1), F32)
    pieces = [None] * tiles
    for t in reversed(range(tiles)):
        own = suffix[rows * t : rows * t + rows]
        pieces[t] = own + later
        later = later + own[:, :1]
    weight = jnp.exp(z + jnp.concatenate(pieces, axis=1)).astype(BF16)
    out = jnp.dot(weight, kv_ref[...], preferred_element_type=F32)
    out_ref[0] = out[:group, HEAD_DIM:].astype(BF16)
    for copy in copies:
        copy.wait()


def read(off, mine, other, q):
    blocks, half, width = mine.shape
    span = 2 * blocks * half
    group = q.shape[1]
    return pl.pallas_call(
        read_kernel,
        out_shape=(jax.ShapeDtypeStruct((1, 1, span, width), BF16), jax.ShapeDtypeStruct(q.shape, BF16)),
        in_specs=[SMEM, VMEM, VMEM, VMEM],
        out_specs=(HBM, VMEM),
        scratch_shapes=[pltpu.VMEM((span, width), BF16), pltpu.SemaphoreType.DMA((PARTS,))],
        compiler_params=GRANT,
        cost_estimate=pl.CostEstimate(flops=32 * span * width, bytes_accessed=4 << 20, transcendentals=24 * span),
    )(off, mine, other, q)


def local(mixer_input, key_weight, content_projection_matrix, new_queries, head_stick_offset):
    seqs, block, width = mixer_input.shape
    depth, columns = key_weight.shape
    half = block // 2
    other = [(0, 1), (1, 0)]
    rows = mixer_input.reshape(seqs * block, width)
    their_rows = lax.ppermute(rows, "core", other)
    pair = jnp.stack([key_weight, content_projection_matrix])
    shape = [2 if name == "core" else 1 for name in WEIGHT_ORDER]
    weight = jnp.broadcast_to(pair.reshape(*shape, depth, columns), (2, 2, 2, depth, columns)).reshape(8, depth, columns)
    weight = lax.all_to_all(weight, WEIGHT_ORDER, 0, 0, tiled=True)
    packed = project(rows, their_rows, weight, seqs, half)
    packed = lax.all_to_all(packed, CHIP_ORDER, 0, 0, tiled=True)
    held = (*(name.replace("x", "z") for name in CHIP_ORDER), "y2", "y1", "y0")
    packed = packed.reshape(2, 2, 2, 2, 2, half, 128).transpose(*(held.index(n) for n in ORDER), 5, 6).reshape(-1, half, 128)
    mine = lax.all_to_all(packed, ORDER, 0, 0, tiled=True)
    theirs = lax.ppermute(mine, "core", other)
    return read(head_stick_offset, mine, theirs, new_queries)


def solution(mesh):
    wide = Mesh(mesh.devices.reshape([2] * 9), ("gr", *BITS, *LINE, "core"))
    sp, tp = BITS, (*LINE, "core")
    return jax.shard_map(
        local,
        mesh=wide,
        in_specs=(P(("gr", *tp), sp, None), P(tp, None), P(tp, None), P(("gr", *sp), tp, None), P()),
        out_specs=(P(("gr", *sp), tp, None, None), P(("gr", *sp), tp, None)),
        check_vma=False,
    )
```
